32 devices in a mesh: ep: 8 (over z, y), tp: 4 (over x, core).
Axes of the slice: x: 2, y: 2, z: 4, core: 2. Of those that a mesh axis runs over, the one named last changes fastest.
Arguments:
- tokens: bfloat16 [1344, 2048], P('ep'), may hold values from -6 to 6
- cotangent: bfloat16 [1344, 2048], P('ep'), may hold values from -6 to 6
- group_ids: int32 [1344, 1], P('ep'), may hold values from 0 to 7; in each aligned block of 168 rows (0 to 167, 168 to 335, ...) at most 32 rows name the same one
- within_ids: int32 [1344, 2], P('ep'), may hold values from 0 to 1, all different within a row
- gate_weights: bfloat16 [1344, 2], P('ep'), may hold values from 0.099609375 to 1
- w_gate: bfloat16 [16, 2048, 1024], P('ep', None, 'tp'), may hold values from -0.125 to 0.125
- w_up: bfloat16 [16, 2048, 1024], P('ep', None, 'tp'), may hold values from -0.125 to 0.125
- w_down: bfloat16 [16, 1024, 2048], P('ep', 'tp'), may hold values from -0.1875 to 0.1875
Outputs:
- tokens_grad: bfloat16 [1344, 2048], P('ep', 'tp')
- gate_grad: float32 [1344, 2], P('ep')
- w_gate_grad: bfloat16 [16, 2048, 1024], P('ep', None, 'tp')
- w_up_grad: bfloat16 [16, 2048, 1024], P('ep', None, 'tp')
- w_down_grad: bfloat16 [16, 1024, 2048], P('ep', 'tp')
The draws below stay inside these ranges and needn't reach their ends.
Inputs may be any that keep to these rules, and one draw needn't show every extreme that they name: `group_ids`: in the rows of one device no group is chosen by more than 32 rows. `within_ids`: the two entries of a row differ.
All inputs are finite; a program needn't handle non-finite values.
Results may differ from the reference program's by a relative error of at most 0.017.
Values may be sent and summed in bfloat16 or wider, within the bound.
No kernel may reach another device: no remote copies, remote signals or barrier semaphores. Data moves between devices by JAX's collectives and lax.ppermute only.
A program may use at most 64 MiB of HBM per device.

```python
import math
import jax
import jax.numpy as jnp
import numpy as np
from jax import lax

D = 2048
FF = 1024
GROUP_EXPERTS = 2
TOP_K = 2
TOK_DEV = 168
GROUPS = 8
EXPERTS = 16
CAP = 32
TOKENS = 1344
N_EP = 8
N_TP = 4


def steps_of(stream_key, shape, shards, least, largest):
    loudness, own = 1.0, jax.random.fold_in(stream_key, 6)
    for position, shards_of in shards:
        steps = jnp.exp(jax.random.uniform(jax.random.fold_in(own, position), (shards_of,), jnp.float32, least / len(shards), largest / len(shards)))
        loudness = loudness * jnp.repeat(steps, shape[position] // shards_of).reshape([-1 if axis == position else 1 for axis in range(len(shape))])
    return loudness


def different_ones(stream_key, rows, number_of, top, lift):
    ranking = jax.random.permutation(jax.random.fold_in(stream_key, 1), number_of)
    pull = ranking
    for power in range(3):
        pull = pull * pull // number_of
    pull = pull * lift // number_of
    tickets = jax.random.randint(jax.random.fold_in(stream_key, 2), (rows, number_of), 0, 4096) + pull
    sure = jax.random.permutation(jax.random.fold_in(stream_key, 3), rows)[jnp.arange(number_of) % rows]
    tickets = jnp.where(jnp.arange(rows)[:, None] == sure[None, :], 1 << 14, tickets)
    score = tickets * number_of + jnp.arange(number_of)
    return lax.top_k(score.astype(jnp.int32), top)[1].astype(jnp.int32)


def routed_block(rng, own, number, rows, count, top, bound, lean):
    ranking = jax.random.permutation(rng, count)
    packed, usual = portions_of(count, rows * top, bound, lean, True), portions_of(count, rows * top, bound, lean, False)
    places = jnp.arange(count)

    def named(sizes, turn):
        used = int((sizes > 0).sum())
        fixed = max(1, used // 4)
        moved = fixed + (places - fixed + turn * (used - fixed)) % max(1, count - fixed)
        return jnp.zeros((count,), jnp.int32).at[ranking[jnp.where(places < fixed, places, moved)]].set(jnp.asarray(sizes, jnp.int32))

    sizes = jnp.where(number % 4 == 0, named(packed, number // 4), named(usual, number - number // 4 - 1))
    mixed = jax.random.permutation(jax.random.fold_in(own, 3), count)
    source_of, receiver = mixed[0:count // 2 * 2:2], mixed[1:count // 2 * 2:2]
    margin = jnp.minimum(sizes[source_of] - 1, bound - sizes[receiver]) // 2
    margin = jnp.where((source_of == ranking[0]) | (receiver == ranking[0]) | (sizes[receiver] == 0), 0, jnp.maximum(margin, 0))
    moved = jax.random.randint(jax.random.fold_in(own, 4), (count // 2,), 0, 1 << 20) % (margin + 1)
    sizes = sizes.at[source_of].add(-moved).at[receiver].add(moved)
    items = jnp.searchsorted(jnp.cumsum(sizes), jnp.arange(rows * top), side="right").astype(jnp.int32)
    grid = items.reshape(top, rows).T
    grid = grid[jax.random.permutation(jax.random.fold_in(own, 1), rows)]
    turn = jax.random.randint(jax.random.fold_in(own, 2), (rows, 1), 0, top)
    return jnp.take_along_axis(grid, (jnp.arange(top)[None, :] + turn) % top, axis=1)


def portions_of(number_of, total, bound, lean, full):
    loads = [(1 << 20) // math.isqrt(rank ** lean) + 1 for rank in range(1, number_of + 1)]
    largest = bound if full else min(bound, max(-(-total // number_of), total * loads[0] // sum(loads)))
    least = 1 if total - largest >= number_of - 1 else 0
    counts, spare = [largest] + [least] * (number_of - 1), total - largest - least * (number_of - 1)
    while spare > 0:
        free = [i for i in range(1, number_of) if counts[i] < largest] or [i for i in range(1, number_of) if counts[i] < bound]
        mass, remaining = sum([loads[i] for i in free]), spare
        for i in free:
            more = min(bound - counts[i], max(1, remaining * loads[i] // mass), spare)
            counts[i] = counts[i] + more
            spare = spare - more
    return np.array(counts)


def noise(stream_key, dims, spread, bound, pieces=(), kind=jnp.bfloat16):
    gain = steps_of(stream_key, dims, pieces, -0.22, 0.18) if pieces else 1.0
    array = jax.random.normal(stream_key, dims, jnp.float32) * spread * gain
    return jnp.minimum(jnp.maximum(array, -bound), bound).astype(kind)


def setup_inputs(seed: int = 0) -> dict:
    splits = jax.random.split(jax.random.key(seed), 9)
    tokens = noise(splits[0], (TOKENS, D), 1.0, 6.0, ((0, 8),))
    cotangent = noise(splits[1], (TOKENS, D), 1.0, 6.0, ((0, 8),))
    group_ids_keys = jax.random.split(jax.random.fold_in(splits[2], 1), TOKENS // TOK_DEV)
    group_ids_turns = jax.random.permutation(jax.random.fold_in(splits[2], 3), TOKENS // TOK_DEV)
    group_ids = jax.vmap(lambda own, number: routed_block(jax.random.fold_in(splits[2], 2), own, number, TOK_DEV, GROUPS, 1, CAP, 2))(group_ids_keys, group_ids_turns).reshape((TOKENS, 1))
    within_ids = different_ones(splits[3], TOKENS, GROUP_EXPERTS, TOP_K, 8192)
    gate_weights = jnp.clip(jnp.exp(math.log(1.0) - 2.306499 * jax.random.uniform(splits[4], (TOKENS, TOP_K), jnp.float32) ** steps_of(splits[4], (TOKENS, TOP_K), ((0, 8),), -0.2, 0.2)), 0.099609375, 1.0).astype(jnp.bfloat16)
    w_gate = noise(splits[5], (EXPERTS, D, FF), D ** -0.5, 0.125, ((0, 8), (2, 4)))
    w_up = noise(splits[6], (EXPERTS, D, FF), D ** -0.5, 0.125, ((0, 8), (2, 4)))
    w_down = noise(splits[7], (EXPERTS, FF, D), FF ** -0.5, 0.1875, ((0, 8), (1, 4)))
    return {"tokens": tokens, "cotangent": cotangent, "group_ids": group_ids, "within_ids": within_ids, "gate_weights": gate_weights, "w_gate": w_gate, "w_up": w_up, "w_down": w_down}


def reference(tokens, cotangent, group_ids, within_ids, gate_weights, w_gate, w_up, w_down):
    rows_max = N_EP * CAP
    ff_local = FF // N_TP
    group_of = group_ids[:, 0]
    sorted_rows = jnp.argsort(group_of, stable=True).astype(jnp.int32)
    in_group = (group_of[:, None] == jnp.arange(GROUPS, dtype=jnp.int32)[None, :]).astype(jnp.int32)
    group_counts = jnp.sum(in_group, axis=0)
    offsets = jnp.cumsum(group_counts) - group_counts
    local_ids = jnp.arange(GROUP_EXPERTS, dtype=jnp.int32)
    chosen = (within_ids[:, :, None] == local_ids[None, None, :]).astype(jnp.float32)
    combine = jnp.sum(chosen * gate_weights.astype(jnp.float32)[:, :, None], axis=1).astype(jnp.bfloat16)

    def one_group(group_index):
        positions = jnp.arange(rows_max, dtype=jnp.int32)
        is_valid = positions < group_counts[group_index]
        row_ids = sorted_rows[jnp.clip(offsets[group_index] + positions, 0, TOKENS - 1)]
        keep = is_valid[:, None]
        slot_x = jnp.where(keep, tokens[row_ids], jnp.zeros((), jnp.bfloat16))
        slot_dy = jnp.where(keep, cotangent[row_ids], jnp.zeros((), jnp.bfloat16))
        slot_comb = jnp.where(keep, combine[row_ids], jnp.zeros((), jnp.bfloat16))
        first = (group_index * GROUP_EXPERTS).astype(jnp.int32)
        local_gate = lax.dynamic_slice_in_dim(w_gate, first, GROUP_EXPERTS, 0)
        local_up = lax.dynamic_slice_in_dim(w_up, first, GROUP_EXPERTS, 0)
        local_down = lax.dynamic_slice_in_dim(w_down, first, GROUP_EXPERTS, 0)
        dy_float = slot_dy.astype(jnp.float32)
        blocks = jnp.zeros((N_TP, rows_max, D), jnp.float32)
        gate_parts = []
        grads_gate = []
        grads_up = []
        grads_down = []
        for expert in range(GROUP_EXPERTS):
            pre_gate = jnp.dot(slot_x, local_gate[expert], preferred_element_type=jnp.float32)
            pre_up = jnp.dot(slot_x, local_up[expert], preferred_element_type=jnp.float32)
            sig_gate = jax.nn.sigmoid(pre_gate)
            act_b = (pre_gate * sig_gate * pre_up).astype(jnp.bfloat16)
            down = jnp.dot(act_b, local_down[expert], preferred_element_type=jnp.float32)
            gate_parts.append(jnp.sum(dy_float * down, axis=1))
            scaled = (slot_comb[:, expert:expert + 1].astype(jnp.float32) * dy_float).astype(jnp.bfloat16)
            grads_down.append(jnp.dot(act_b.T, scaled, preferred_element_type=jnp.float32).astype(jnp.bfloat16))
            act_grad = jnp.dot(scaled, local_down[expert].T, preferred_element_type=jnp.float32)
            gate_b = (act_grad * pre_up * sig_gate * (1.0 + pre_gate * (1.0 - sig_gate))).astype(jnp.bfloat16)
            up_b = (act_grad * pre_gate * sig_gate).astype(jnp.bfloat16)
            grads_gate.append(jnp.dot(slot_x.T, gate_b, preferred_element_type=jnp.float32).astype(jnp.bfloat16))
            grads_up.append(jnp.dot(slot_x.T, up_b, preferred_element_type=jnp.float32).astype(jnp.bfloat16))
            gate_split = gate_b.astype(jnp.float32).reshape(rows_max, N_TP, ff_local)
            up_split = up_b.astype(jnp.float32).reshape(rows_max, N_TP, ff_local)
            wg_split = local_gate[expert].astype(jnp.float32).reshape(D, N_TP, ff_local)
            wu_split = local_up[expert].astype(jnp.float32).reshape(D, N_TP, ff_local)
            blocks = blocks + jnp.einsum('rnf,dnf->nrd', gate_split, wg_split)
            blocks = blocks + jnp.einsum('rnf,dnf->nrd', up_split, wu_split)
        rounded = lax.optimization_barrier(blocks.astype(jnp.bfloat16)).astype(jnp.float32)
        dx_rows = jnp.sum(rounded, axis=0).astype(jnp.bfloat16)
        return (dx_rows, jnp.stack(gate_parts, axis=1), row_ids, is_valid,
                jnp.stack(grads_gate), jnp.stack(grads_up), jnp.stack(grads_down))

    dx_all, gate_all, rows_all, valid_all, gg_all, gu_all, gd_all = lax.map(
        one_group, jnp.arange(GROUPS, dtype=jnp.int32))
    flat_rows = rows_all.reshape(-1)
    flat_valid = valid_all.reshape(-1)[:, None]
    dx_flat = jnp.where(flat_valid, dx_all.reshape(-1, D).astype(jnp.float32), 0.0)
    tokens_grad = jnp.zeros((TOKENS, D), jnp.float32).at[flat_rows].add(dx_flat).astype(jnp.bfloat16)
    gate_flat = jnp.where(flat_valid, gate_all.reshape(-1, GROUP_EXPERTS), 0.0)
    dense_gate = jnp.zeros((TOKENS, GROUP_EXPERTS), jnp.float32).at[flat_rows].add(gate_flat)
    gate_grad = jnp.sum(chosen * dense_gate[:, None, :], axis=2)
    w_gate_grad = gg_all.reshape(EXPERTS, D, FF)
    w_up_grad = gu_all.reshape(EXPERTS, D, FF)
    w_down_grad = gd_all.reshape(EXPERTS, FF, D)
    return tokens_grad, gate_grad, w_gate_grad, w_up_grad, w_down_grad
```

```python
import functools

import jax
import jax.numpy as jnp
from jax import lax
from jax.experimental import pallas as pl
from jax.experimental.pallas import tpu as pltpu
from jax.sharding import PartitionSpec as P


LANES = 128
AXES = ("ep", "tp")
BF16 = jnp.bfloat16
F32 = jnp.float32
TRANS_LHS = (((0,), (0,)), ((), ()))
TRANS_RHS = (((1,), (1,)), ((), ()))
VMEM = pl.BlockSpec(memory_space=pltpu.VMEM)


def partner(ep, e, s):
    if ep & (ep - 1) == 0:
        return e ^ s
    return (s - e + ep) % ep


def params(mib):
    return pltpu.CompilerParams(vmem_limit_bytes=mib << 20)


def dot(a, b, dims=(((1,), (0,)), ((), ()))):
    return lax.dot_general(a, b, dims, preferred_element_type=F32)


def iota(shape, axis):
    return lax.broadcasted_iota(jnp.int32, shape, axis)


def place_kernel(ep, tp, nk, cap, experts, tok, cot, group, within, weight, target, *outs):
    e, t = lax.axis_index("ep"), lax.axis_index("tp")
    rows, width = tok.shape
    group_of = group[...]
    member = group_of == iota((rows, ep), 1)
    earlier = (iota((rows, rows), 0) > iota((rows, rows), 1)).astype(F32).astype(BF16)
    before = dot(earlier, member.astype(F32).astype(BF16))
    rank = jnp.sum(jnp.where(member, before, 0.0), axis=1, keepdims=True).astype(jnp.int32)
    spot = group_of * cap + rank
    target[...] = spot
    lane = iota((rows, LANES), 1)
    comb = jnp.zeros((rows, LANES), F32)
    for k in range(weight.shape[1]):
        comb = comb + jnp.where(within[:, k : k + 1] == lane, weight[:, k : k + 1].astype(F32), 0.0)
    comb = jnp.where(lane < experts, comb, 0.0).astype(BF16)
    for k in range(nk):
        here = spot - partner(ep, e, k * tp + t) * cap
        pick = (here == iota((rows, cap), 1)).astype(F32).astype(BF16)
        outs[k][:, :width] = dot(pick, tok[...], TRANS_LHS).astype(BF16)
        outs[k][:, width : 2 * width] = dot(pick, cot[...], TRANS_LHS).astype(BF16)
        outs[k][:, 2 * width :] = dot(pick, comb, TRANS_LHS).astype(BF16)


def expert_kernel(nb, cap, *refs):
    blocks, (wg, wu, wd) = refs[:nb], refs[nb : nb + 3]
    keep, send, act_out, gate_out, up_out, xs, dys, cs = refs[nb + 3 :]
    experts, width, hidden = wg.shape
    for j, block in enumerate(blocks):
        rows = slice(j * cap, (j + 1) * cap)
        xs[rows, :] = block[:, :width]
        dys[rows, :] = block[:, width : 2 * width]
        cs[rows, :] = block[:, 2 * width :]
    half = nb * cap // 2
    lane = iota((nb * cap, LANES), 1)
    gate_sum = jnp.zeros((nb * cap, LANES), F32)
    for e in range(experts):
        cols = slice(e * hidden, (e + 1) * hidden)
        pre_gate = dot(xs[...], wg[e])
        pre_up = dot(xs[...], wu[e])
        back = dot(dys[...], wd[e], TRANS_RHS)
        sig = jax.nn.sigmoid(pre_gate)
        silu = pre_gate * sig
        act = silu * pre_up
        scale = cs[:, e : e + 1].astype(F32)
        total = jnp.sum(act * back, axis=1, keepdims=True)
        gate_sum = gate_sum + jnp.where(lane == e, total, 0.0)
        act_grad = scale * back
        act_out[:, cols] = (scale * act).astype(BF16)
        gate_out[:, cols] = (act_grad * pre_up * sig * (1.0 + pre_gate * (1.0 - sig))).astype(BF16)
        up_out[:, cols] = (act_grad * silu).astype(BF16)
    gate_sum = gate_sum.astype(BF16)
    keep[:, width:] = gate_sum[:half]
    send[:, width:] = gate_sum[half:]
    step = min(width, 256)
    for n in range(width // step):
        ns = slice(n * step, (n + 1) * step)
        acc = jnp.zeros((nb * cap, step), F32)
        for e in range(experts):
            cols = slice(e * hidden, (e + 1) * hidden)
            acc = acc + dot(gate_out[:, cols], wg[e, ns, :], TRANS_RHS)
            acc = acc + dot(up_out[:, cols], wu[e, ns, :], TRANS_RHS)
        acc = acc.astype(BF16)
        keep[:, ns] = acc[:half]
        send[:, ns] = acc[half:]


def up_grad_kernel(nk, tp, cap, width, step, *refs):
    n = nk * tp
    blocks, gates, ups = refs[:n], refs[n : n + nk], refs[n + nk : n + 2 * nk]
    wg_out, wu_out, xs, gs, us = refs[n + 2 * nk :]
    i = pl.program_id(0)
    experts, _, hidden = wg_out.shape

    @pl.when(i == 0)
    def _():
        for j, block in enumerate(blocks):
            xs[j * cap : (j + 1) * cap, :] = block[:, :width]
        for k in range(nk):
            rows = slice(k * tp * cap, (k + 1) * tp * cap)
            gs[rows, :] = gates[k][...]
            us[rows, :] = ups[k][...]

    x = xs[:, pl.ds(pl.multiple_of(i * step, step), step)]
    for e in range(experts):
        cols = slice(e * hidden, (e + 1) * hidden)
        wg_out[e] = dot(x, gs[:, cols], TRANS_LHS).astype(BF16)
        wu_out[e] = dot(x, us[:, cols], TRANS_LHS).astype(BF16)


def down_grad_kernel(nk, tp, cap, width, step, *refs):
    n = nk * tp
    blocks, acts = refs[:n], refs[n : n + nk]
    wd_out, dys, hs = refs[n + nk :]
    i = pl.program_id(0)
    experts, hidden, _ = wd_out.shape

    @pl.when(i == 0)
    def _():
        for j, block in enumerate(blocks):
            dys[j * cap : (j + 1) * cap, :] = block[:, width : 2 * width]
        for k in range(nk):
            hs[k * tp * cap : (k + 1) * tp * cap, :] = acts[k][...]

    dy = dys[:, pl.ds(pl.multiple_of(i * step, step), step)]
    for e in range(experts):
        cols = slice(e * hidden, (e + 1) * hidden)
        wd_out[e] = dot(hs[:, cols], dy, TRANS_LHS).astype(BF16)


def add_core_kernel(width, bit, keep, recv, total, send):
    t = lax.axis_index("tp")
    total[...] = (keep[...].astype(F32) + recv[...].astype(F32)).astype(BF16)
    half = width // 2
    other = pl.multiple_of((1 - lax.rem(lax.div(t, bit), 2)) * half, half)
    send[:, :half] = total[:, pl.ds(other, half)]
    send[:, half:] = total[:, width:]


def add_far_kernel(width, bit, order, cap, total, recv, *outs):
    t = lax.axis_index("tp")
    half = width // 2
    mine = pl.multiple_of(lax.rem(lax.div(t, bit), 2) * half, half)
    for j, other in enumerate(order):
        rows, theirs = slice(j * cap, (j + 1) * cap), slice(other * cap, (other + 1) * cap)
        own = total[rows, pl.ds(mine, half)].astype(F32)
        outs[j][:, :half] = (own + recv[theirs, :half].astype(F32)).astype(BF16)
        own = total[rows, width:].astype(F32)
        outs[j][:, half:] = (own + recv[theirs, half:].astype(F32)).astype(BF16)


def final_kernel(ep, tp, nk, cap, rels, *refs):
    nb = nk * len(rels) * 2
    blocks = refs[:nb]
    target, within, tok_out, gate_out, data, gates = refs[nb:]
    e, t = lax.axis_index("ep"), lax.axis_index("tp")
    rows, share = tok_out.shape
    start = pl.multiple_of(lax.rem(t, 2) * share, share)
    spot = target[...]
    picks = []
    j = 0
    for k in range(nk):
        for rel in rels:
            for core in range(2):
                at = slice(j * cap, (j + 1) * cap)
                data[at, :] = blocks[j][:, pl.ds(start, share)]
                gates[at, :] = blocks[j][:, 2 * share :]
                owner = partner(ep, e, k * tp + ((t ^ rel) ^ core))
                picks.append(spot - owner * cap == iota((rows, cap), 1))
                j += 1
    pick = jnp.concatenate([p.astype(F32) for p in picks], axis=1).astype(BF16)
    tok_out[...] = dot(pick, data[...]).astype(BF16)
    dense = dot(pick, gates[...])
    cols = iota(within.shape, 1)
    result = jnp.zeros(within.shape, F32)
    lane = iota(dense.shape, 1)
    for k in range(within.shape[1]):
        value = jnp.sum(jnp.where(lane == within[:, k : k + 1], dense, 0.0), axis=1, keepdims=True)
        result = result + jnp.where(cols == k, value, 0.0)
    gate_out[...] = result


def on_device(tokens, cotangent, group_ids, within_ids, gate_weights, w_gate, w_up, w_down):
    ep, tp = lax.axis_size("ep"), lax.axis_size("tp")
    rows, width = tokens.shape
    experts, _, hidden = w_gate.shape
    cap = (3 * rows + 2 * ep - 1) // (2 * ep)
    nk = ep // tp
    assert nk * tp == ep and tp & (tp - 1) == 0 and tp >= 4
    far_bits = [1 << b for b in range(1, tp.bit_length() - 1)]

    def struct(*shape, dtype=BF16):
        return jax.ShapeDtypeStruct(shape, dtype)

    def over_tp(x, bit):
        return lax.ppermute(
            x, AXES, [(e * tp + t, e * tp + (t ^ bit)) for e in range(ep) for t in range(tp)]
        )

    def over_ep(x, k, rel):
        return lax.ppermute(
            x,
            AXES,
            [
                (e * tp + t, partner(ep, e, k * tp + (t ^ rel)) * tp + t)
                for e in range(ep)
                for t in range(tp)
            ],
        )

    packed = 2 * width + LANES
    target, *outgoing = pl.pallas_call(
        functools.partial(place_kernel, ep, tp, nk, cap, experts),
        out_shape=[struct(rows, 1, dtype=jnp.int32)] + [struct(cap, packed)] * nk,
        in_specs=[VMEM] * 5,
        out_specs=[VMEM] * (nk + 1),
        compiler_params=params(12),
        cost_estimate=pl.CostEstimate(
            flops=4 * rows * nk * cap * width, bytes_accessed=4 * rows * width, transcendentals=0
        ),
        name="place",
    )(tokens, cotangent, group_ids, within_ids, gate_weights)

    gathered = []
    rels = [0]
    arrived = [over_ep(outgoing[k], k, 0) for k in range(nk)]
    for k in range(nk):
        blocks, rels = [arrived[k]], [0]
        for bit in far_bits + [1]:
            blocks = blocks + [over_tp(b, bit) for b in blocks]
            rels = rels + [r ^ bit for r in rels]
        gathered.append(blocks)
    row_rels = rels[: tp // 2]

    near = tp // 2 * cap
    total_rows = tp * cap
    acts, gates, ups, returned = [], [], [], []
    for k in range(nk):
        keep, send, act, gate, up = pl.pallas_call(
            functools.partial(expert_kernel, tp, cap),
            out_shape=[struct(near, width + LANES)] * 2 + [struct(total_rows, experts * hidden)] * 3,
            in_specs=[VMEM] * (tp + 3),
            out_specs=[VMEM] * 5,
            scratch_shapes=[
                pltpu.VMEM((total_rows, width), BF16),
                pltpu.VMEM((total_rows, width), BF16),
                pltpu.VMEM((total_rows, LANES), BF16),
            ],
            compiler_params=params(12),
            cost_estimate=pl.CostEstimate(
                flops=10 * total_rows * width * hidden * experts,
                bytes_accessed=6 * experts * width * hidden,
                transcendentals=total_rows * hidden * experts,
            ),
            name="experts",
        )(*gathered[k], w_gate, w_up, w_down)
        acts.append(act)
        gates.append(gate)
        ups.append(up)
        recv = over_tp(send, 1)
        have = width
        bits = far_bits[::-1]
        total, send = pl.pallas_call(
            functools.partial(add_core_kernel, have, bits[0]),
            out_shape=[struct(near, have + LANES), struct(near, have // 2 + LANES)],
            in_specs=[VMEM] * 2,
            out_specs=[VMEM] * 2,
            compiler_params=params(8),
            name="add_core",
        )(keep, recv)
        for i, bit in enumerate(bits):
            recv = over_tp(send, bit)
            order = [row_rels.index(r ^ bit) for r in row_rels]
            parts = pl.pallas_call(
                functools.partial(add_far_kernel, have, bit, order, cap),
                out_shape=[struct(cap, have // 2 + LANES)] * len(row_rels),
                in_specs=[VMEM] * 2,
                out_specs=[VMEM] * len(row_rels),
                compiler_params=params(8),
                name="add_far",
            )(total, recv)
            have //= 2
            if i + 1 < len(bits):
                total = jnp.concatenate(parts, axis=0)
                half = have // 2
                other = (1 - lax.rem(lax.div(lax.axis_index("tp"), bits[i + 1]), 2)) * half
                send = jnp.concatenate(
                    [lax.dynamic_slice_in_dim(total, other, half, 1), total[:, have:]], axis=1
                )
        for part, rel in zip(parts, row_rels):
            back = over_ep(part, k, rel)
            returned += [back, over_tp(back, 1)]

    blocks = [b for group in gathered for b in group]
    step = min(width, 512)
    whole = pl.BlockSpec(memory_space=pltpu.VMEM)
    w_gate_grad, w_up_grad = pl.pallas_call(
        functools.partial(up_grad_kernel, nk, tp, cap, width, step),
        out_shape=[struct(experts, width, hidden)] * 2,
        grid=(width // step,),
        in_specs=[whole] * (len(blocks) + 2 * nk),
        out_specs=[pl.BlockSpec((experts, step, hidden), lambda i: (0, i, 0))] * 2,
        scratch_shapes=[
            pltpu.VMEM((nk * total_rows, width), BF16),
            pltpu.VMEM((nk * total_rows, experts * hidden), BF16),
            pltpu.VMEM((nk * total_rows, experts * hidden), BF16),
        ],
        compiler_params=params(20),
        cost_estimate=pl.CostEstimate(
            flops=4 * nk * total_rows * width * hidden * experts,
            bytes_accessed=4 * experts * width * hidden,
            transcendentals=0,
        ),
        name="up_grad",
    )(*blocks, *gates, *ups)
    w_down_grad = pl.pallas_call(
        functools.partial(down_grad_kernel, nk, tp, cap, width, step),
        out_shape=struct(experts, hidden, width),
        grid=(width // step,),
        in_specs=[whole] * (len(blocks) + nk),
        out_specs=pl.BlockSpec((experts, hidden, step), lambda i: (0, 0, i)),
        scratch_shapes=[
            pltpu.VMEM((nk * total_rows, width), BF16),
            pltpu.VMEM((nk * total_rows, experts * hidden), BF16),
        ],
        compiler_params=params(20),
        cost_estimate=pl.CostEstimate(
            flops=2 * nk * total_rows * width * hidden * experts,
            bytes_accessed=2 * experts * width * hidden,
            transcendentals=0,
        ),
        name="down_grad",
    )(*blocks, *acts)

    share = width // tp
    tokens_grad, gate_grad = pl.pallas_call(
        functools.partial(final_kernel, ep, tp, nk, cap, row_rels),
        out_shape=[struct(rows, share), struct(rows, within_ids.shape[1], dtype=F32)],
        in_specs=[VMEM] * (len(returned) + 2),
        out_specs=[VMEM] * 2,
        scratch_shapes=[
            pltpu.VMEM((len(returned) * cap, share), BF16),
            pltpu.VMEM((len(returned) * cap, LANES), BF16),
        ],
        compiler_params=params(8),
        name="collect",
    )(*returned, target, within_ids)
    return tokens_grad, gate_grad, w_gate_grad, w_up_grad, w_down_grad


def solution(mesh):
    in_specs = (
        P("ep", None),
        P("ep", None),
        P("ep", None),
        P("ep", None),
        P("ep", None),
        P("ep", None, "tp"),
        P("ep", None, "tp"),
        P("ep", "tp", None),
    )
    out_specs = (
        P("ep", "tp"),
        P("ep", None),
        P("ep", None, "tp"),
        P("ep", None, "tp"),
        P("ep", "tp", None),
    )
    return jax.shard_map(
        on_device, mesh=mesh, in_specs=in_specs, out_specs=out_specs, check_vma=False
    )
```

```python
import functools

import jax
import jax.numpy as jnp
from jax import lax
from jax.experimental import pallas as pl
from jax.experimental.pallas import tpu as pltpu
from jax.sharding import PartitionSpec as P


LANES = 128
AXES = ("ep", "tp")
BF16 = jnp.bfloat16
F32 = jnp.float32
TRANS_LHS = (((0,), (0,)), ((), ()))
TRANS_RHS = (((1,), (1,)), ((), ()))
VMEM = pl.BlockSpec(memory_space=pltpu.VMEM)
HBM = pl.BlockSpec(memory_space=pltpu.HBM)


def partner(ep, e, s):
    if ep & (ep - 1) == 0:
        return e ^ s
    return (s - e + ep) % ep


def shift(tp, k, t):
    core = t % 2
    turn = core * (tp // 2) + ((t // 2) ^ (core * (tp // 2 - 1)))
    return k * tp + (turn if k % 2 == 0 else tp - 1 - turn)


def params(mib):
    return pltpu.CompilerParams(vmem_limit_bytes=mib << 20)


def dot(a, b, dims=(((1,), (0,)), ((), ()))):
    return lax.dot_general(a, b, dims, preferred_element_type=F32)


def iota(shape, axis):
    return lax.broadcasted_iota(jnp.int32, shape, axis)


def place_kernel(
    ep, tp, nk, cap, split, tok_hbm, cot_hbm, group_hbm, within_hbm, weight_hbm, spot_out, *refs
):
    n = sum(2 if cut else 1 for cut in split)
    outs, (tok, cot, group, within, weight, sems) = refs[:n], refs[n:]
    pairs = [
        (group_hbm, group),
        (within_hbm, within),
        (weight_hbm, weight),
        (tok_hbm, tok),
        (cot_hbm, cot),
    ]
    copies = [pltpu.make_async_copy(a, b, sems.at[i]) for i, (a, b) in enumerate(pairs)]
    for copy in copies:
        copy.start()
    for copy in copies[:3]:
        copy.wait()
    e, t = lax.axis_index("ep"), lax.axis_index("tp")
    rows, width = tok.shape
    group_of = group[...]
    member = group_of == iota((ep, rows), 0)
    earlier = (iota((rows, rows), 0) < iota((rows, rows), 1)).astype(F32).astype(BF16)
    before = dot(member.astype(F32).astype(BF16), earlier)
    rank = jnp.sum(jnp.where(member, before, 0.0), axis=0, keepdims=True).astype(jnp.int32)
    spot = group_of * cap + rank
    spot_out[...] = spot
    slot = iota((LANES, rows), 0)
    comb = jnp.zeros((LANES, rows), F32)
    for k in range(weight.shape[0]):
        comb = comb + jnp.where(within[k : k + 1, :] == slot, weight[k : k + 1, :].astype(F32), 0.0)
    comb = comb.astype(BF16)
    picks = []
    for k in range(nk):
        here = spot - partner(ep, e, shift(tp, k, t)) * cap
        picks.append((here == iota((cap, rows), 0)).astype(F32).astype(BF16))
    outs, firsts, seconds = list(outs), [], []
    for cut in split:
        firsts.append(outs.pop(0))
        seconds.append(outs.pop(0) if cut else firsts[-1])
    for pick, second in zip(picks, seconds):
        second[:, second.shape[1] - LANES :] = dot(pick, comb, TRANS_RHS).astype(BF16)
    copies[3].wait()
    for pick, first in zip(picks, firsts):
        first[:, :width] = dot(pick, tok[...]).astype(BF16)
    copies[4].wait()
    for pick, second in zip(picks, seconds):
        second[:, cotangent_at(second, width)] = dot(pick, cot[...]).astype(BF16)


def cotangent_at(block, width):
    end = block.shape[1] - LANES
    return slice(end - width, end)


def load_kernel(*refs):
    n = (len(refs) - 1) // 2
    sems = refs[-1]
    copies = [
        pltpu.make_async_copy(refs[i].at[e], refs[n + i].at[e], sems.at[i, e])
        for i in range(n)
        for e in range(refs[i].shape[0])
    ]
    for copy in copies:
        copy.start()
    for copy in copies:
        copy.wait()


def expert_kernel(nb, cap, *refs):
    firsts, seconds, (wg, wu, wd) = refs[:nb], refs[nb : 2 * nb], refs[2 * nb : 2 * nb + 3]
    keep, send, act_out, gate_out, up_out, xs, dys, cs = refs[2 * nb + 3 :]
    experts, width, hidden = wg.shape
    for j, (first, second) in enumerate(zip(firsts, seconds)):
        rows = slice(j * cap, (j + 1) * cap)
        xs[rows, :] = first[:, :width]
        dys[rows, :] = second[:, cotangent_at(second, width)]
        cs[rows, :] = second[:, second.shape[1] - LANES :]
    half = nb * cap // 2
    lane = iota((nb * cap, LANES), 1)
    gate_sum = jnp.zeros((nb * cap, LANES), F32)
    for e in range(experts):
        cols = slice(e * hidden, (e + 1) * hidden)
        pre_gate = dot(xs[...], wg[e])
        pre_up = dot(xs[...], wu[e])
        back = dot(dys[...], wd[e], TRANS_RHS)
        sig = jax.nn.sigmoid(pre_gate)
        silu = pre_gate * sig
        act = silu * pre_up
        scale = cs[:, e : e + 1].astype(F32)
        total = jnp.sum(act * back, axis=1, keepdims=True)
        gate_sum = gate_sum + jnp.where(lane == e, total, 0.0)
        act_grad = scale * back
        act_out[:, cols] = (scale * act).astype(BF16)
        gate_out[:, cols] = (act_grad * pre_up * sig * (1.0 + pre_gate * (1.0 - sig))).astype(BF16)
        up_out[:, cols] = (act_grad * silu).astype(BF16)
    gate_sum = gate_sum.astype(BF16)
    keep[:, width:] = gate_sum[:half]
    send[:, width:] = gate_sum[half:]
    step = min(width, 256)
    for n in range(width // step):
        ns = slice(n * step, (n + 1) * step)
        acc = jnp.zeros((nb * cap, step), F32)
        for e in range(experts):
            cols = slice(e * hidden, (e + 1) * hidden)
            acc = acc + dot(gate_out[:, cols], wg[e, ns, :], TRANS_RHS)
            acc = acc + dot(up_out[:, cols], wu[e, ns, :], TRANS_RHS)
        acc = acc.astype(BF16)
        keep[:, ns] = acc[:half]
        send[:, ns] = acc[half:]


def up_grad_kernel(nk, tp, cap, width, step, *refs):
    n = nk * tp
    blocks, gates, ups = refs[:n], refs[n : n + nk], refs[n + nk : n + 2 * nk]
    wg_out, wu_out, xs, gs, us = refs[n + 2 * nk :]
    i = pl.program_id(0)
    experts, _, hidden = wg_out.shape

    @pl.when(i == 0)
    def _():
        for j, block in enumerate(blocks):
            xs[j * cap : (j + 1) * cap, :] = block[:, :width]
        for k in range(nk):
            rows = slice(k * tp * cap, (k + 1) * tp * cap)
            gs[rows, :] = gates[k][...]
            us[rows, :] = ups[k][...]

    x = xs[:, pl.ds(pl.multiple_of(i * step, step), step)]
    for e in range(experts):
        cols = slice(e * hidden, (e + 1) * hidden)
        wg_out[e] = dot(x, gs[:, cols], TRANS_LHS).astype(BF16)
        wu_out[e] = dot(x, us[:, cols], TRANS_LHS).astype(BF16)


def down_grad_kernel(nk, tp, cap, width, step, *refs):
    n = nk * tp
    blocks, acts = refs[:n], refs[n : n + nk]
    wd_out, dys, hs = refs[n + nk :]
    i = pl.program_id(0)
    experts, hidden, _ = wd_out.shape

    @pl.when(i == 0)
    def _():
        for j, block in enumerate(blocks):
            dys[j * cap : (j + 1) * cap, :] = block[:, cotangent_at(block, width)]
        for k in range(nk):
            hs[k * tp * cap : (k + 1) * tp * cap, :] = acts[k][...]

    dy = dys[:, pl.ds(pl.multiple_of(i * step, step), step)]
    for e in range(experts):
        cols = slice(e * hidden, (e + 1) * hidden)
        wd_out[e] = dot(hs[:, cols], dy, TRANS_LHS).astype(BF16)


def add_core_kernel(width, bit, cap, keep, recv, total, *sends):
    t = lax.axis_index("tp")
    total[...] = (keep[...].astype(F32) + recv[...].astype(F32)).astype(BF16)
    half = width // 2
    other = pl.multiple_of((1 - lax.rem(lax.div(t, bit), 2)) * half, half)
    for j, send in enumerate(sends):
        rows = slice(j * cap, (j + 1) * cap)
        send[:, :half] = total[rows, pl.ds(other, half)]
        send[:, half:] = total[rows, width:]


def add_far_kernel(width, bit, rows, total, recv, out):
    t = lax.axis_index("tp")
    half = width // 2
    mine = pl.multiple_of(lax.rem(lax.div(t, bit), 2) * half, half)
    own = total[rows, pl.ds(mine, half)].astype(F32)
    out[:, :half] = (own + recv[:, :half].astype(F32)).astype(BF16)
    own = total[rows, width:].astype(F32)
    out[:, half:] = (own + recv[:, half:].astype(F32)).astype(BF16)


def final_kernel(ep, tp, nk, cap, rels, *refs):
    nb = nk * len(rels) * 2
    blocks = refs[:nb]
    spot_ref, within, tok_out, gate_out, data, gates = refs[nb:]
    e, t = lax.axis_index("ep"), lax.axis_index("tp")
    rows, share = tok_out.shape
    start = pl.multiple_of(lax.rem(t, 2) * share, share)
    spot = spot_ref[...]
    picks = []
    j = 0
    for k in range(nk):
        for rel in rels:
            for core in range(2):
                at = slice(j * cap, (j + 1) * cap)
                data[at, :] = blocks[j][:, pl.ds(start, share)]
                gates[at, :] = blocks[j][:, 2 * share :]
                owner = partner(ep, e, shift(tp, k, (t ^ rel) ^ core))
                picks.append((spot - owner * cap == iota((cap, rows), 0)).astype(F32))
                j += 1
    pick = jnp.concatenate(picks, axis=0).astype(BF16)
    tok_out[...] = dot(pick, data[...], TRANS_LHS).astype(BF16)
    dense = dot(gates[...], pick, TRANS_LHS)
    lane = iota(dense.shape, 0)
    for k in range(within.shape[0]):
        gate_out[k : k + 1, :] = jnp.sum(
            jnp.where(lane == within[k : k + 1, :], dense, 0.0), axis=0, keepdims=True
        )


def on_device(tokens, cotangent, group_ids, within_ids, gate_weights, w_gate, w_up, w_down):
    ep, tp = lax.axis_size("ep"), lax.axis_size("tp")
    rows, width = tokens.shape
    experts, _, hidden = w_gate.shape
    cap = (3 * rows + 2 * ep - 1) // (2 * ep)
    nk = ep // tp
    assert nk * tp == ep and tp & (tp - 1) == 0 and tp >= 4
    far_bits = [1 << b for b in range(1, tp.bit_length() - 1)]

    def struct(*shape, dtype=BF16):
        return jax.ShapeDtypeStruct(shape, dtype)

    def over_tp(x, bit):
        pairs = [(e * tp + t, e * tp + (t ^ bit)) for e in range(ep) for t in range(tp)]
        return lax.ppermute(x, AXES, pairs)

    def over_ep(x, k, rel):
        pairs = [
            (e * tp + t, partner(ep, e, shift(tp, k, t ^ rel)) * tp + t)
            for e in range(ep)
            for t in range(tp)
        ]
        return lax.ppermute(x, AXES, pairs)

    def kernel(*args, **options):
        return pl.pallas_call(*args, **options)

    split = [k % 2 == 1 for k in range(nk)]
    shapes = [
        struct(cap, columns)
        for cut in split
        for columns in ((width, width + LANES) if cut else (2 * width + LANES,))
    ]
    groups, chosen, weights = group_ids.T, within_ids.T, gate_weights.T

    def in_hbm(x):
        return pltpu.with_memory_space_constraint(x, pltpu.HBM)

    spot, *outgoing = kernel(
        functools.partial(place_kernel, ep, tp, nk, cap, split),
        out_shape=[struct(1, rows, dtype=jnp.int32)] + shapes,
        in_specs=[HBM] * 5,
        out_specs=[VMEM] * (len(shapes) + 1),
        scratch_shapes=[
            pltpu.VMEM((rows, width), BF16),
            pltpu.VMEM((rows, width), BF16),
            pltpu.VMEM(groups.shape, groups.dtype),
            pltpu.VMEM(chosen.shape, chosen.dtype),
            pltpu.VMEM(weights.shape, weights.dtype),
            pltpu.SemaphoreType.DMA((5,)),
        ],
        compiler_params=params(12),
        cost_estimate=pl.CostEstimate(
            flops=4 * rows * nk * cap * width, bytes_accessed=4 * rows * width, transcendentals=0
        ),
    )(*map(in_hbm, (tokens, cotangent, groups, chosen, weights)))
    held = kernel(
        load_kernel,
        out_shape=[struct(*w.shape) for w in (w_gate, w_up, w_down)],
        in_specs=[HBM] * 3,
        out_specs=[VMEM] * 3,
        scratch_shapes=[pltpu.SemaphoreType.DMA((3, experts))],
        compiler_params=params(2),
        cost_estimate=pl.CostEstimate(
            flops=1 << 30, bytes_accessed=6 * experts * width * hidden, transcendentals=0
        ),
    )(*map(in_hbm, (w_gate, w_up, w_down)))

    names = [f"{k}{part}" for k in range(nk) for part in ("xy" if split[k] else "x")]
    arrived = {name: over_ep(block, int(name[:-1]), 0) for name, block in zip(names, outgoing)}
    gathered = {}
    for name, block in arrived.items():
        blocks, rels = [block], [0]
        for bit in far_bits + [1]:
            blocks = blocks + [over_tp(b, bit) for b in blocks]
            rels = rels + [r ^ bit for r in rels]
        gathered[name] = blocks
    firsts = [gathered[f"{k}x"] for k in range(nk)]
    seconds = [gathered[f"{k}y" if split[k] else f"{k}x"] for k in range(nk)]
    row_rels = rels[: tp // 2]

    near = tp // 2 * cap
    total_rows = tp * cap
    acts, gates, ups, returned = [], [], [], []
    for k in range(nk):
        keep, send, act, gate, up = kernel(
        functools.partial(expert_kernel, tp, cap),
            out_shape=[struct(near, width + LANES)] * 2 + [struct(total_rows, experts * hidden)] * 3,
            in_specs=[VMEM] * (2 * tp + 3),
            out_specs=[VMEM] * 5,
            scratch_shapes=[
                pltpu.VMEM((total_rows, width), BF16),
                pltpu.VMEM((total_rows, width), BF16),
                pltpu.VMEM((total_rows, LANES), BF16),
            ],
            compiler_params=params(12),
            cost_estimate=pl.CostEstimate(
                flops=10 * total_rows * width * hidden * experts,
                bytes_accessed=6 * experts * width * hidden,
                transcendentals=total_rows * hidden * experts,
            ),
        )(*firsts[k], *seconds[k], *held)
        acts.append(act)
        gates.append(gate)
        ups.append(up)
        recv = over_tp(send, 1)
        have = width
        bits = far_bits[::-1]
        count = len(row_rels)
        total, *sends = kernel(
            functools.partial(add_core_kernel, have, bits[0], cap),
            out_shape=[struct(near, have + LANES)] + [struct(cap, have // 2 + LANES)] * count,
            in_specs=[VMEM] * 2,
            out_specs=[VMEM] * (count + 1),
            compiler_params=params(8),
        )(keep, recv)
        for i, bit in enumerate(bits):
            order = [row_rels.index(r ^ bit) for r in row_rels]
            received = [over_tp(send, bit) for send in sends]
            parts = [
                kernel(
                    functools.partial(
                        add_far_kernel, have, bit, slice(j * cap, (j + 1) * cap)
                    ),
                    out_shape=struct(cap, have // 2 + LANES),
                    in_specs=[VMEM] * 2,
                    out_specs=VMEM,
                    compiler_params=params(8),
                )(total, received[order[j]])
                for j in range(count)
            ]
            have //= 2
            if i + 1 < len(bits):
                total = jnp.concatenate(parts, axis=0)
                half = have // 2
                other = (1 - lax.rem(lax.div(lax.axis_index("tp"), bits[i + 1]), 2)) * half
                sends = [
                    jnp.concatenate(
                        [lax.dynamic_slice_in_dim(part, other, half, 1), part[:, have:]], axis=1
                    )
                    for part in parts
                ]
        for part, rel in zip(parts, row_rels):
            back = over_ep(part, k, rel)
            returned += [back, over_tp(back, 1)]

    first_blocks = [b for group in firsts for b in group]
    second_blocks = [b for group in seconds for b in group]
    step = min(width, 512)
    whole = pl.BlockSpec(memory_space=pltpu.VMEM)
    w_gate_grad, w_up_grad = kernel(
        functools.partial(up_grad_kernel, nk, tp, cap, width, step),
        out_shape=[struct(experts, width, hidden)] * 2,
        grid=(width // step,),
        in_specs=[whole] * (ep + 2 * nk),
        out_specs=[pl.BlockSpec((experts, step, hidden), lambda i: (0, i, 0))] * 2,
        scratch_shapes=[
            pltpu.VMEM((nk * total_rows, width), BF16),
            pltpu.VMEM((nk * total_rows, experts * hidden), BF16),
            pltpu.VMEM((nk * total_rows, experts * hidden), BF16),
        ],
        compiler_params=params(20),
        cost_estimate=pl.CostEstimate(
            flops=4 * nk * total_rows * width * hidden * experts,
            bytes_accessed=4 * experts * width * hidden,
            transcendentals=0,
        ),
    )(*first_blocks, *gates, *ups)
    w_down_grad = kernel(
        functools.partial(down_grad_kernel, nk, tp, cap, width, step),
        out_shape=struct(experts, hidden, width),
        grid=(width // step,),
        in_specs=[whole] * (ep + nk),
        out_specs=pl.BlockSpec((experts, hidden, step), lambda i: (0, 0, i)),
        scratch_shapes=[
            pltpu.VMEM((nk * total_rows, width), BF16),
            pltpu.VMEM((nk * total_rows, experts * hidden), BF16),
        ],
        compiler_params=params(20),
        cost_estimate=pl.CostEstimate(
            flops=2 * nk * total_rows * width * hidden * experts,
            bytes_accessed=2 * experts * width * hidden,
            transcendentals=0,
        ),
    )(*second_blocks, *acts)

    share = width // tp
    tokens_grad, gate_grad = kernel(
        functools.partial(final_kernel, ep, tp, nk, cap, row_rels),
        out_shape=[struct(rows, share), struct(within_ids.shape[1], rows, dtype=F32)],
        in_specs=[VMEM] * (len(returned) + 2),
        out_specs=[VMEM] * 2,
        scratch_shapes=[
            pltpu.VMEM((len(returned) * cap, share), BF16),
            pltpu.VMEM((len(returned) * cap, LANES), BF16),
        ],
        compiler_params=params(8),
    )(*returned, spot, chosen)
    return tokens_grad, gate_grad.T, w_gate_grad, w_up_grad, w_down_grad


def solution(mesh):
    in_specs = (
        P("ep", None),
        P("ep", None),
        P("ep", None),
        P("ep", None),
        P("ep", None),
        P("ep", None, "tp"),
        P("ep", None, "tp"),
        P("ep", "tp", None),
    )
    out_specs = (
        P("ep", "tp"),
        P("ep", None),
        P("ep", None, "tp"),
        P("ep", None, "tp"),
        P("ep", "tp", None),
    )

    return jax.shard_map(
        on_device, mesh=mesh, in_specs=in_specs, out_specs=out_specs, check_vma=False
    )
```
